32 devices in a mesh: sp: 16 (over z, y, x), tp: 2 (over core).
Axes of the slice: x: 2, y: 2, z: 4, core: 2. Of those that a mesh axis runs over, the one named last changes fastest.
Arguments:
- query_rows: bfloat16 [4096, 1024], P('sp', 'tp'), may hold values from -26 to 26
- key_rows: bfloat16 [4096, 128], P('sp', 'tp'), may hold values from -26 to 26
- value_head_rows: bfloat16 [4096, 128], P('sp', 'tp'), may hold values from -6 to 6
- sink_logit_head: float32 [16], P('tp'), may hold values from -6 to 6
- out_weight: bfloat16 [1024, 2048], P('tp'), may hold values from -0.1875 to 0.1875
- residual: bfloat16 [4096, 2048], P(('sp', 'tp')), may hold values from -6 to 6
- norm_gain: float32 [2048], replicated, may hold values from 0.1 to 1.9
- routes: int32 [4096, 2], P(('sp', 'tp')), may hold values from 0 to 15, all different within a row; in each aligned block of 128 rows (0 to 127, 128 to 255, ...) at most 24 rows name the same one
- route_weights: float32 [4096, 2], P(('sp', 'tp')), may hold values from 0.1 to 1
- gate_proj: bfloat16 [16, 2048, 3584], P('sp', None, 'tp'), may hold values from -0.125 to 0.125
- up_proj: bfloat16 [16, 2048, 3584], P('sp', None, 'tp'), may hold values from -0.125 to 0.125
- down_proj: bfloat16 [16, 3584, 2048], P('sp', 'tp'), may hold values from -0.09375 to 0.09375
Outputs:
- output: bfloat16 [4096, 2048], P(('sp', 'tp'))
The draws below stay inside these ranges and needn't reach their ends.
Inputs may be any that keep to these rules, and one draw needn't show every extreme that they name: `routes`: A row names 2 different experts. Among the rows of one device no expert is named more than 24 times, a bound that some block reaches on some devices.
All inputs are finite; a program needn't handle non-finite values.
Results may differ from the reference program's by a relative error of at most 0.0055.
Values may be sent and summed in bfloat16 or wider, within the bound.
No kernel may reach another device: no remote copies, remote signals or barrier semaphores. Data moves between devices by JAX's collectives and lax.ppermute only.
A program may use at most 128 MiB of HBM per device.

```python
import math
import jax
import jax.numpy as jnp
import numpy as np
from jax import lax

D = 2048
QUERY_HEADS = 16
KEY_VALUE_HEADS = 2
HEAD_SIZE = 64
FF = 3584
TOP = 2
WINDOW_KEYS = 128
TOKENS_PER_SHARD = 256
SEQUENCE_TOKENS = 4096
ROWS_DEV = 128
EXPERTS = 16
CAP = 24
N_SP = 16
N_TP = 2


def draw_query_rows(key, part):
    start_offset = jnp.clip(jax.random.normal(jax.random.fold_in(key, 1), (SEQUENCE_TOKENS, QUERY_HEADS * HEAD_SIZE), jnp.float32), -6.0, 6.0)
    return start_offset.astype(jnp.bfloat16)


def draw_key_rows(key, part):
    start_offset = jnp.clip(jax.random.normal(jax.random.fold_in(key, 2), (SEQUENCE_TOKENS, KEY_VALUE_HEADS * HEAD_SIZE), jnp.float32), -6.0, 6.0)
    return start_offset.astype(jnp.bfloat16)


def shard_levels(stream_key, extent, pieces, least, top_value):
    gain, own = 1.0, jax.random.fold_in(stream_key, 6)
    for dim, parts in pieces:
        draws = jnp.exp(jax.random.uniform(jax.random.fold_in(own, dim), (parts,), jnp.float32, least / len(pieces), top_value / len(pieces)))
        gain = gain * jnp.repeat(draws, extent[dim] // parts).reshape([-1 if axis == dim else 1 for axis in range(len(extent))])
    return gain


def routed_block(key, own, number, rows, count, top, reach, lean):
    ranking = jax.random.permutation(key, count)
    heavy_load, ordinary = load_shares(count, rows * top, reach, lean, True), load_shares(count, rows * top, reach, lean, False)
    places = jnp.arange(count)

    def named(tallies, offset_by):
        used = int((tallies > 0).sum())
        fixed = max(1, used // 4)
        shifted = fixed + (places - fixed + offset_by * (used - fixed)) % max(1, count - fixed)
        return jnp.zeros((count,), jnp.int32).at[ranking[jnp.where(places < fixed, places, shifted)]].set(jnp.asarray(tallies, jnp.int32))

    tallies = jnp.where(number % 4 == 0, named(heavy_load, number // 4), named(ordinary, number - number // 4 - 1))
    mixed = jax.random.permutation(jax.random.fold_in(own, 3), count)
    giver, receiver = mixed[0:count // 2 * 2:2], mixed[1:count // 2 * 2:2]
    slack = jnp.minimum(tallies[giver] - 1, reach - tallies[receiver]) // 2
    slack = jnp.where((giver == ranking[0]) | (receiver == ranking[0]) | (tallies[receiver] == 0), 0, jnp.maximum(slack, 0))
    shifted = jax.random.randint(jax.random.fold_in(own, 4), (count // 2,), 0, 1 << 20) % (slack + 1)
    tallies = tallies.at[giver].add(-shifted).at[receiver].add(shifted)
    items = jnp.searchsorted(jnp.cumsum(tallies), jnp.arange(rows * top), side="right").astype(jnp.int32)
    table = items.reshape(top, rows).T
    table = table[jax.random.permutation(jax.random.fold_in(own, 1), rows)]
    offset_by = jax.random.randint(jax.random.fold_in(own, 2), (rows, 1), 0, top)
    return jnp.take_along_axis(table, (jnp.arange(top)[None, :] + offset_by) % top, axis=1)


def load_shares(count, total, limit, lean, full):
    loads = [(1 << 20) // math.isqrt(standing ** lean) + 1 for standing in range(1, count + 1)]
    largest = limit if full else min(limit, max(-(-total // count), total * loads[0] // sum(loads)))
    least = 1 if total - largest >= count - 1 else 0
    holding, surplus = [largest] + [least] * (count - 1), total - largest - least * (count - 1)
    while surplus > 0:
        candidates = [i for i in range(1, count) if holding[i] < largest] or [i for i in range(1, count) if holding[i] < limit]
        mass, remaining = sum([loads[i] for i in candidates]), surplus
        for i in candidates:
            addition = min(limit - holding[i], max(1, remaining * loads[i] // mass), surplus)
            holding[i] = holding[i] + addition
            surplus = surplus - addition
    return np.array(holding)


def normal_values(rng, dims, spread, limit, shards=(), kind=jnp.bfloat16):
    array = jax.random.normal(rng, dims, jnp.float32) * spread
    if len(shards) > 0:
        array = shard_levels(rng, dims, shards, -0.22, 0.18) * array
    return jnp.clip(array, min=-limit, max=limit).astype(kind)


def setup_inputs(seed: int = 0) -> dict:
    key_list = jax.random.split(jax.random.key(seed), 13)
    query_rows = draw_query_rows(jax.random.fold_in(key_list[12], 71), 0)
    key_rows = draw_key_rows(jax.random.fold_in(key_list[12], 71), 0)
    value_head_rows = normal_values(key_list[2], (SEQUENCE_TOKENS, KEY_VALUE_HEADS * HEAD_SIZE), 1.0, 6.0, ((0, 16), (1, 2)))
    sink_logit_head = normal_values(key_list[3], (QUERY_HEADS,), 2.0, 6.0, ((0, 2),), jnp.float32)
    out_weight = normal_values(key_list[4], (QUERY_HEADS * HEAD_SIZE, D), (QUERY_HEADS * HEAD_SIZE) ** -0.5, 0.1875, ((0, 2),))
    residual = normal_values(key_list[5], (SEQUENCE_TOKENS, D), 1.0, 6.0, ((0, 32),))
    norm_gain = jnp.clip(1.0 + 0.18 * jax.random.normal(key_list[6], (D,), jnp.float32), 0.1, 1.9)
    routes_keys = jax.random.split(jax.random.fold_in(key_list[7], 1), SEQUENCE_TOKENS // ROWS_DEV)
    routes_turns = jax.random.permutation(jax.random.fold_in(key_list[7], 3), SEQUENCE_TOKENS // ROWS_DEV)
    routes = jax.vmap(lambda own, number: routed_block(jax.random.fold_in(key_list[7], 2), own, number, ROWS_DEV, EXPERTS, TOP, CAP, 2))(routes_keys, routes_turns).reshape((SEQUENCE_TOKENS, TOP))
    route_weights = jnp.clip(0.1 + 0.9 * jax.random.uniform(key_list[8], (SEQUENCE_TOKENS, TOP), jnp.float32) ** shard_levels(key_list[8], (SEQUENCE_TOKENS, TOP), ((0, 32),), -0.2, 0.2), 0.1, 1.0)
    gate_proj = normal_values(key_list[9], (EXPERTS, D, FF), D ** -0.5, 0.125, ((0, 16), (2, 2)))
    up_proj = normal_values(key_list[10], (EXPERTS, D, FF), D ** -0.5, 0.125, ((0, 16), (2, 2)))
    down_proj = normal_values(key_list[11], (EXPERTS, FF, D), FF ** -0.5, 0.09375, ((0, 16), (1, 2)))
    return {"query_rows": query_rows, "key_rows": key_rows, "value_head_rows": value_head_rows, "sink_logit_head": sink_logit_head, "out_weight": out_weight, "residual": residual, "norm_gain": norm_gain, "routes": routes, "route_weights": route_weights, "gate_proj": gate_proj, "up_proj": up_proj, "down_proj": down_proj}


def attention_all(query_rows, key_rows, value_head_rows, sink_logit_head):
    query_group = QUERY_HEADS // KEY_VALUE_HEADS
    blocks = SEQUENCE_TOKENS // TOKENS_PER_SHARD
    leading_edge = jnp.zeros((WINDOW_KEYS, KEY_VALUE_HEADS * HEAD_SIZE), jnp.bfloat16)
    key_pad = jnp.concatenate([leading_edge, key_rows], axis=0)
    value_pad = jnp.concatenate([leading_edge, value_head_rows], axis=0)
    slope_values = jnp.exp2(-8.0 * jnp.arange(1, QUERY_HEADS + 1, dtype=jnp.float32) / QUERY_HEADS).reshape(KEY_VALUE_HEADS, query_group)
    sink_portion = sink_logit_head.astype(jnp.float32).reshape(KEY_VALUE_HEADS, query_group)[:, :, None]

    def attend(block):
        start = (block * TOKENS_PER_SHARD).astype(jnp.int32)
        query_vector = lax.dynamic_slice_in_dim(query_rows, start, TOKENS_PER_SHARD, 0).astype(jnp.float32)
        key_block = lax.dynamic_slice_in_dim(key_pad, start, TOKENS_PER_SHARD + WINDOW_KEYS, 0).astype(jnp.float32)
        value_block = lax.dynamic_slice_in_dim(value_pad, start, TOKENS_PER_SHARD + WINDOW_KEYS, 0).astype(jnp.float32)
        score_matrix = jnp.einsum('rjwh,cjh->jwrc', query_vector.reshape(TOKENS_PER_SHARD, KEY_VALUE_HEADS, query_group, HEAD_SIZE), key_block.reshape(-1, KEY_VALUE_HEADS, HEAD_SIZE)) * HEAD_SIZE ** (-0.5)
        query_pos = start + jnp.arange(TOKENS_PER_SHARD, dtype=jnp.int32)
        key_pos = start - WINDOW_KEYS + jnp.arange(TOKENS_PER_SHARD + WINDOW_KEYS, dtype=jnp.int32)
        distance = query_pos[:, None] - key_pos[None, :]
        inside = (distance >= 0) & (distance < WINDOW_KEYS) & (key_pos[None, :] >= 0)
        score_matrix = score_matrix - slope_values[:, :, None, None] * distance.astype(jnp.float32)[None, None]
        score_matrix = jnp.where(inside[None, None], score_matrix, -jnp.inf)
        peak = jnp.maximum(lax.optimization_barrier(jnp.max(score_matrix, axis=-1)), sink_portion)
        expd = jnp.exp(score_matrix - peak[..., None])
        denom = lax.optimization_barrier(jnp.sum(expd, axis=-1)) + jnp.exp(sink_portion - peak)
        probabilities = (expd / denom[..., None]).astype(jnp.bfloat16)
        final_output = jnp.einsum('wfbt,twj->bwfj', probabilities.astype(jnp.float32), value_block.reshape(-1, KEY_VALUE_HEADS, HEAD_SIZE))
        return final_output.reshape(TOKENS_PER_SHARD, QUERY_HEADS * HEAD_SIZE).astype(jnp.bfloat16)
    outs = lax.map(attend, jnp.arange(blocks, dtype=jnp.int32))
    return outs.reshape(SEQUENCE_TOKENS, QUERY_HEADS * HEAD_SIZE)

def reference(query_rows, key_rows, value_head_rows, sink_logit_head, out_weight, residual, norm_gain, routes, route_weights, gate_proj, up_proj, down_proj):
    attended = attention_all(query_rows, key_rows, value_head_rows, sink_logit_head)
    mixed = residual.astype(jnp.float32) + jnp.dot(attended, out_weight, preferred_element_type=jnp.float32)
    scale = lax.rsqrt(lax.optimization_barrier(jnp.mean(mixed * mixed, axis=-1, keepdims=True)) + 1e-05)
    normed = (mixed * scale * norm_gain).astype(jnp.bfloat16)
    devices = N_SP * N_TP
    per_dev = ROWS_DEV * TOP
    chosen = routes.reshape(devices, per_dev).astype(jnp.int32)
    onehot = (chosen[:, :, None] == jnp.arange(EXPERTS, dtype=jnp.int32)[None, None, :]).astype(jnp.int32)
    running = jnp.cumsum(onehot, axis=1).astype(jnp.int32)
    rank_in = (lax.optimization_barrier(jnp.sum(onehot * running, axis=-1)) - 1).astype(jnp.int32)
    source = jnp.arange(devices, dtype=jnp.int32)[:, None]
    slot_index = ((chosen * devices + source) * CAP + rank_in).astype(jnp.int32)
    token_of = (source * ROWS_DEV + jnp.arange(per_dev, dtype=jnp.int32)[None, :] // TOP).astype(jnp.int32)
    slots_all = EXPERTS * devices * CAP
    table = jnp.full((slots_all,), SEQUENCE_TOKENS, jnp.int32).at[slot_index.reshape(-1)].set(token_of.reshape(-1))
    normed_pad = jnp.concatenate([normed, jnp.zeros((1, D), jnp.bfloat16)], axis=0)
    half = FF // 2

    def expert(index):
        picks = lax.dynamic_slice_in_dim(table, (index * devices * CAP).astype(jnp.int32), devices * CAP, 0)
        rows_in = normed_pad[picks]
        gate = jnp.dot(rows_in, gate_proj[index], preferred_element_type=jnp.float32)
        upper = jnp.dot(rows_in, up_proj[index], preferred_element_type=jnp.float32)
        hidden = (jax.nn.silu(gate) * upper).astype(jnp.bfloat16)
        down = down_proj[index]
        first = jnp.dot(hidden[:, :half], down[:half], preferred_element_type=jnp.float32).astype(jnp.bfloat16)
        second = jnp.dot(hidden[:, half:], down[half:], preferred_element_type=jnp.float32).astype(jnp.bfloat16)
        first, second = lax.optimization_barrier((first, second))
        return (first.astype(jnp.float32) + second.astype(jnp.float32)).astype(jnp.bfloat16)
    results = lax.map(expert, jnp.arange(EXPERTS, dtype=jnp.int32)).reshape(slots_all, D)
    picked = results[slot_index.reshape(-1)].reshape(SEQUENCE_TOKENS, TOP, D)
    moe_sum = lax.optimization_barrier(jnp.sum(route_weights[:, :, None] * picked.astype(jnp.float32), axis=1))
    return (mixed + moe_sum).astype(jnp.bfloat16)
```

```python
import jax
import jax.numpy as jnp
from jax import lax
from jax.sharding import PartitionSpec as P

QUERY_HEADS = 16
KEY_VALUE_HEADS = 2
HEAD_SIZE = 64
TOP = 2
WINDOW_KEYS = 128


def from_behind(block, axis, distance):
    devices = range(lax.axis_size(axis))
    route = [(i - distance, i) for i in devices if i - distance in devices]
    return lax.ppermute(block, axis, route)


def swap_cores(block):
    return lax.ppermute(block, "tp", [(0, 1), (1, 0)])


def attend(query_rows, key_rows, value_head_rows, sink_logit_head):
    length = query_rows.shape[0]
    query_group = QUERY_HEADS // KEY_VALUE_HEADS
    width = key_rows.shape[1]
    local_kv = width // HEAD_SIZE
    local_heads = local_kv * query_group
    sp_index = lax.axis_index("sp")
    tp_index = lax.axis_index("tp")
    tail = jnp.concatenate(
        [key_rows[length - WINDOW_KEYS :], value_head_rows[length - WINDOW_KEYS :]], axis=1
    )
    before = from_behind(tail, "sp", 1)
    key_all = jnp.concatenate([before[:, :width], key_rows], axis=0)
    value_all = jnp.concatenate([before[:, width:], value_head_rows], axis=0)
    score_matrix = jnp.einsum(
        "rjwh,cjh->jwrc",
        query_rows.reshape(length, local_kv, query_group, HEAD_SIZE),
        key_all.reshape(-1, local_kv, HEAD_SIZE),
        preferred_element_type=jnp.float32,
    ) * HEAD_SIZE ** (-0.5)
    query_pos = sp_index * length + jnp.arange(length, dtype=jnp.int32)
    key_pos = sp_index * length - WINDOW_KEYS + jnp.arange(length + WINDOW_KEYS, dtype=jnp.int32)
    distance = query_pos[:, None] - key_pos[None, :]
    inside = (distance >= 0) & (distance < WINDOW_KEYS) & (key_pos[None, :] >= 0)
    head_ids = (tp_index * local_heads + jnp.arange(local_heads, dtype=jnp.int32)).astype(
        jnp.float32
    )
    slope_values = jnp.exp2(-8.0 * (head_ids + 1.0) / QUERY_HEADS).reshape(local_kv, query_group)
    score_matrix = (
        score_matrix - slope_values[:, :, None, None] * distance.astype(jnp.float32)[None, None]
    )
    score_matrix = jnp.where(inside[None, None], score_matrix, -jnp.inf)
    sink_portion = sink_logit_head.reshape(local_kv, query_group)[:, :, None]
    peak = jnp.maximum(jnp.max(score_matrix, axis=-1), sink_portion)
    expd = jnp.exp(score_matrix - peak[..., None])
    denom = jnp.sum(expd, axis=-1) + jnp.exp(sink_portion - peak)
    probabilities = (expd / denom[..., None]).astype(jnp.bfloat16)
    return (
        jnp.einsum(
            "wfbt,twj->bwfj",
            probabilities,
            value_all.reshape(-1, local_kv, HEAD_SIZE),
            preferred_element_type=jnp.float32,
        )
        .reshape(length, local_heads * HEAD_SIZE)
        .astype(jnp.bfloat16)
    )


def on_device(
    query_rows,
    key_rows,
    value_head_rows,
    sink_logit_head,
    out_weight,
    residual,
    norm_gain,
    routes,
    route_weights,
    gate_proj,
    up_proj,
    down_proj,
):
    n_sp = lax.axis_size("sp")
    tp_index = lax.axis_index("tp")
    length = query_rows.shape[0]
    own_rows = residual.shape[0]
    width = residual.shape[1]
    other_weight = swap_cores(out_weight)
    attended = attend(query_rows, key_rows, value_head_rows, sink_logit_head)
    mine = lax.dynamic_slice_in_dim(attended, tp_index * own_rows, own_rows, 0)
    theirs = lax.dynamic_slice_in_dim(attended, (1 - tp_index) * own_rows, own_rows, 0)
    from_other = swap_cores(theirs)
    mixed = (
        residual.astype(jnp.float32)
        + jnp.dot(mine, out_weight, preferred_element_type=jnp.float32)
        + jnp.dot(from_other, other_weight, preferred_element_type=jnp.float32)
    )
    scale = lax.rsqrt(jnp.mean(mixed * mixed, axis=-1, keepdims=True) + 1e-05)
    normed = (mixed * scale * norm_gain).astype(jnp.bfloat16)
    capacity = 3 * own_rows * TOP // (2 * n_sp)
    chosen = routes.reshape(-1)
    onehot = chosen[:, None] == jnp.arange(n_sp, dtype=jnp.int32)[None, :]
    pairs = chosen.shape[0]
    order = jnp.arange(pairs, dtype=jnp.int32)
    lower = (order[:, None] > order[None, :]).astype(jnp.bfloat16)
    ahead = jnp.dot(lower, onehot.astype(jnp.bfloat16), preferred_element_type=jnp.float32)
    rank_in = jnp.sum(jnp.where(onehot, ahead, 0.0), axis=1).astype(jnp.int32)
    slot_index = (chosen * capacity + rank_in).reshape(own_rows, TOP)
    slot_ids = jnp.arange(n_sp * capacity, dtype=jnp.int32)
    select = jnp.any(slot_index[None, :, :] == slot_ids[:, None, None], axis=-1)
    dispatch = jnp.dot(
        select.astype(jnp.bfloat16), normed, preferred_element_type=jnp.float32
    ).astype(jnp.bfloat16)
    landed = lax.all_to_all(
        dispatch.reshape(n_sp, capacity, width), "sp", split_axis=0, concat_axis=0, tiled=True
    ).reshape(n_sp * capacity, width)
    rows_in = jnp.concatenate([landed, swap_cores(landed)], axis=0)
    gate = jnp.dot(rows_in, gate_proj[0], preferred_element_type=jnp.float32)
    upper = jnp.dot(rows_in, up_proj[0], preferred_element_type=jnp.float32)
    hidden = (jax.nn.silu(gate) * upper).astype(jnp.bfloat16)
    half = n_sp * capacity
    part_other = jnp.dot(
        hidden[half:], down_proj[0], preferred_element_type=jnp.float32
    ).astype(jnp.bfloat16)
    part_sent = swap_cores(part_other)
    part_own = jnp.dot(
        hidden[:half], down_proj[0], preferred_element_type=jnp.float32
    ).astype(jnp.bfloat16)
    expert_out = (part_own.astype(jnp.float32) + part_sent.astype(jnp.float32)).astype(jnp.bfloat16)
    returned = lax.all_to_all(
        expert_out.reshape(n_sp, capacity, width), "sp", split_axis=0, concat_axis=0, tiled=True
    ).reshape(half, width)
    result = mixed
    for choice in range(TOP):
        pick = (slot_index[:, choice : choice + 1] == slot_ids[None, :]).astype(jnp.bfloat16)
        picked = jnp.dot(pick, returned, preferred_element_type=jnp.float32)
        result = result + route_weights[:, choice : choice + 1] * picked
    return result.astype(jnp.bfloat16)


def solution(mesh):
    placed = (
        P("sp", "tp"),
        P("sp", "tp"),
        P("sp", "tp"),
        P("tp"),
        P("tp", None),
        P(("sp", "tp"), None),
        P(),
        P(("sp", "tp"), None),
        P(("sp", "tp"), None),
        P("sp", None, "tp"),
        P("sp", None, "tp"),
        P("sp", "tp", None),
    )
    return jax.shard_map(
        on_device, mesh=mesh, in_specs=placed, out_specs=P(("sp", "tp"), None), check_vma=False
    )
```

```python
import functools

import jax
import jax.numpy as jnp
from jax import lax
from jax.experimental import pallas as pl
from jax.experimental.pallas import tpu as pltpu
from jax.sharding import PartitionSpec as P


QUERY_HEADS = 16
KEY_VALUE_HEADS = 2
HEAD_SIZE = 64
TOP = 2
WINDOW_KEYS = 128
PLANES = 4


def from_behind(block, axis, distance):
    devices = range(lax.axis_size(axis))
    route = [(i - distance, i) for i in devices if i - distance in devices]
    return lax.ppermute(block, axis, route)


def swap_cores(block):
    return lax.ppermute(block, "tp", [(0, 1), (1, 0)])


def attend(query_rows, key_rows, value_head_rows, sink_logit_head):
    length = query_rows.shape[0]
    query_group = QUERY_HEADS // KEY_VALUE_HEADS
    width = key_rows.shape[1]
    local_kv = width // HEAD_SIZE
    local_heads = local_kv * query_group
    sp_index = lax.axis_index("sp")
    tp_index = lax.axis_index("tp")
    tail = jnp.concatenate(
        [key_rows[length - WINDOW_KEYS :], value_head_rows[length - WINDOW_KEYS :]], axis=1
    )
    before = from_behind(tail, "sp", 1)
    key_all = jnp.concatenate([before[:, :width], key_rows], axis=0)
    value_all = jnp.concatenate([before[:, width:], value_head_rows], axis=0)
    score_matrix = jnp.einsum(
        "rjwh,cjh->jwrc",
        query_rows.reshape(length, local_kv, query_group, HEAD_SIZE),
        key_all.reshape(-1, local_kv, HEAD_SIZE),
        preferred_element_type=jnp.float32,
    ) * HEAD_SIZE ** (-0.5)
    query_pos = sp_index * length + jnp.arange(length, dtype=jnp.int32)
    key_pos = sp_index * length - WINDOW_KEYS + jnp.arange(length + WINDOW_KEYS, dtype=jnp.int32)
    distance = query_pos[:, None] - key_pos[None, :]
    inside = (distance >= 0) & (distance < WINDOW_KEYS) & (key_pos[None, :] >= 0)
    head_ids = (tp_index * local_heads + jnp.arange(local_heads, dtype=jnp.int32)).astype(
        jnp.float32
    )
    slope_values = jnp.exp2(-8.0 * (head_ids + 1.0) / QUERY_HEADS).reshape(local_kv, query_group)
    score_matrix = (
        score_matrix - slope_values[:, :, None, None] * distance.astype(jnp.float32)[None, None]
    )
    score_matrix = jnp.where(inside[None, None], score_matrix, -jnp.inf)
    sink_portion = sink_logit_head.reshape(local_kv, query_group)[:, :, None]
    peak = jnp.maximum(jnp.max(score_matrix, axis=-1), sink_portion)
    expd = jnp.exp(score_matrix - peak[..., None])
    denom = jnp.sum(expd, axis=-1) + jnp.exp(sink_portion - peak)
    probabilities = (expd / denom[..., None]).astype(jnp.bfloat16)
    return (
        jnp.einsum(
            "wfbt,twj->bwfj",
            probabilities,
            value_all.reshape(-1, local_kv, HEAD_SIZE),
            preferred_element_type=jnp.float32,
        )
        .reshape(length, local_heads * HEAD_SIZE)
        .astype(jnp.bfloat16)
    )


BLOCK = 256


def gather_rows(pieces, rows_ref):
    start = 0
    for piece in pieces:
        rows_ref[start : start + piece.shape[0], :] = piece[...]
        start += piece.shape[0]


def expert_body(*refs, count):
    pieces, (gate_ref, up_ref, down_ref, own_ref, other_ref, rows_ref, hidden_ref) = (
        refs[:count],
        refs[count:],
    )
    gather_rows(pieces, rows_ref)
    for start in range(0, gate_ref.shape[1], BLOCK):
        units = slice(start, start + BLOCK)
        rows = rows_ref[...]
        gate = jnp.dot(rows, gate_ref[:, units], preferred_element_type=jnp.float32)
        upper = jnp.dot(rows, up_ref[:, units], preferred_element_type=jnp.float32)
        hidden_ref[:, units] = (gate / (1.0 + jnp.exp(-gate)) * upper).astype(jnp.bfloat16)
    half = own_ref.shape[0]
    for start in range(0, down_ref.shape[1], BLOCK):
        units = slice(start, start + BLOCK)
        part = jnp.dot(
            hidden_ref[...], down_ref[:, units], preferred_element_type=jnp.float32
        ).astype(jnp.bfloat16)
        own_ref[:, units] = part[:half]
        other_ref[:, units] = part[half:]


def expert_parts(pieces, weights):
    width, hidden_units = weights[0].shape
    if any(piece.shape[0] % 8 for piece in pieces):
        pieces = [jnp.concatenate(pieces, axis=0)]
    rows = sum(piece.shape[0] for piece in pieces)
    half = jax.ShapeDtypeStruct((rows // 2, width), jnp.bfloat16)
    inside = pl.BlockSpec(memory_space=pltpu.VMEM)
    return pl.pallas_call(
        functools.partial(expert_body, count=len(pieces)),
        in_specs=[inside] * (len(pieces) + 3),
        out_specs=[inside] * 2,
        out_shape=[half, half],
        scratch_shapes=[
            pltpu.VMEM((rows, width), jnp.bfloat16),
            pltpu.VMEM((rows, hidden_units), jnp.bfloat16),
        ],
        compiler_params=pltpu.CompilerParams(vmem_limit_bytes=8 * 2**20),
        cost_estimate=pl.CostEstimate(
            flops=6 * rows * width * hidden_units,
            transcendentals=rows * hidden_units,
            bytes_accessed=6 * width * hidden_units,
        ),
    )(*pieces, *weights)


def on_device(
    query_rows,
    key_rows,
    value_head_rows,
    sink_logit_head,
    out_weight,
    residual,
    norm_gain,
    routes,
    route_weights,
    gate_proj,
    up_proj,
    down_proj,
):
    n_sp = lax.axis_size("sp")
    tp_index = lax.axis_index("tp")
    own_rows = residual.shape[0]
    width = residual.shape[1]
    other_weight = swap_cores(out_weight)
    attended = attend(query_rows, key_rows, value_head_rows, sink_logit_head)
    mine = lax.dynamic_slice_in_dim(attended, tp_index * own_rows, own_rows, 0)
    theirs = lax.dynamic_slice_in_dim(attended, (1 - tp_index) * own_rows, own_rows, 0)
    from_other = swap_cores(theirs)
    mixed = (
        residual.astype(jnp.float32)
        + jnp.dot(mine, out_weight, preferred_element_type=jnp.float32)
        + jnp.dot(from_other, other_weight, preferred_element_type=jnp.float32)
    )
    scale = lax.rsqrt(jnp.mean(mixed * mixed, axis=-1, keepdims=True) + 1e-05)
    normed = (mixed * scale * norm_gain).astype(jnp.bfloat16)
    plane = n_sp // PLANES
    capacity = 3 * own_rows * TOP // (2 * n_sp)
    group = plane * capacity
    chosen = routes.reshape(-1)
    onehot = chosen[:, None] == jnp.arange(n_sp, dtype=jnp.int32)[None, :]
    pairs = chosen.shape[0]
    order = jnp.arange(pairs, dtype=jnp.int32)
    lower = (order[:, None] > order[None, :]).astype(jnp.bfloat16)
    ahead = jnp.dot(lower, onehot.astype(jnp.bfloat16), preferred_element_type=jnp.float32)
    rank_in = jnp.sum(jnp.where(onehot, ahead, 0.0), axis=1).astype(jnp.int32)
    relative = jnp.bitwise_xor(chosen, lax.axis_index("sp"))
    slot_index = (relative * capacity + rank_in).reshape(own_rows, TOP)

    def ids(number):
        return number * group + jnp.arange(group, dtype=jnp.int32)

    weights = [
        pltpu.with_memory_space_constraint(w[0], pltpu.VMEM)
        for w in (gate_proj, up_proj, down_proj)
    ]

    def selected(number):
        select = jnp.any(slot_index[None, :, :] == ids(number)[:, None, None], axis=-1)
        return jnp.dot(
            select.astype(jnp.bfloat16), normed, preferred_element_type=jnp.float32
        ).astype(jnp.bfloat16)

    def across(block, distance):
        return lax.ppermute(block, "sp", [(i, i ^ distance) for i in range(n_sp)])

    def pieces(block):
        rows = block.shape[0] // plane
        return [block[rows * j : rows * (j + 1)] for j in range(plane)]

    def in_plane(parts):
        return [parts[0]] + [across(parts[j], j) for j in range(1, plane)]

    def expert(parts):
        rows = jnp.concatenate(parts, axis=0) if len(parts) > 1 else parts[0]
        other = swap_cores(rows)
        own_part, other_part = expert_parts([rows, other], weights)
        added = swap_cores(other_part)
        return (own_part.astype(jnp.float32) + added.astype(jnp.float32)).astype(jnp.bfloat16)

    arrived = {number: across(selected(number), number * plane) for number in (3, 1, 2)}
    arrived[0] = selected(0)
    out = {number: expert(in_plane(pieces(arrived[number]))) for number in (0, 3, 1, 2)}
    far_back = in_plane(pieces(across(out[3], 3 * plane)))
    one_back = across(out[1], plane)
    near = [jnp.concatenate(two, axis=0) for two in zip(pieces(out[0]), pieces(one_back))]
    near_back = in_plane(near)
    mid_back = [across(p, 2 * plane + j) for j, p in enumerate(pieces(out[2]))]

    total = jnp.zeros((TOP * own_rows, width), jnp.float32)
    slots = slot_index.T.reshape(-1, 1)
    near_ids = jnp.arange(2 * group, dtype=jnp.int32)
    near_ids = (
        near_ids // capacity % 2 * group
        + near_ids // (2 * capacity) * capacity
        + near_ids % capacity
    )
    groups = ((near_ids, near_back), (ids(3), far_back), (ids(2), mid_back))
    for numbers, back in groups:
        pick = (slots == numbers[None, :]).astype(jnp.bfloat16)
        total = total + jnp.dot(
            pick, jnp.concatenate(back, axis=0), preferred_element_type=jnp.float32
        )
    weighted = route_weights.T.reshape(-1, 1) * total
    return (mixed + jnp.sum(weighted.reshape(TOP, own_rows, width), axis=0)).astype(jnp.bfloat16)


def solution(mesh):
    placed = (
        P("sp", "tp"),
        P("sp", "tp"),
        P("sp", "tp"),
        P("tp"),
        P("tp", None),
        P(("sp", "tp"), None),
        P(),
        P(("sp", "tp"), None),
        P(("sp", "tp"), None),
        P("sp", None, "tp"),
        P("sp", None, "tp"),
        P("sp", "tp", None),
    )

    return jax.shard_map(
        on_device, mesh=mesh, in_specs=placed, out_specs=P(("sp", "tp"), None), check_vma=False
    )
```

```python
import functools

import jax
import jax.numpy as jnp
from jax import lax
from jax.experimental import pallas as pl
from jax.experimental.pallas import tpu as pltpu
from jax.sharding import PartitionSpec as P


QUERY_HEADS = 16
HEAD_SIZE = 64
TOP = 2
WINDOW_KEYS = 128
PLANES = 4


def from_behind(block, axis, distance):
    devices = range(lax.axis_size(axis))
    route = [(i - distance, i) for i in devices if i - distance in devices]
    return lax.ppermute(block, axis, route)


def swap_cores(block):
    return lax.ppermute(block, "tp", [(0, 1), (1, 0)])


INSIDE = pl.BlockSpec(memory_space=pltpu.VMEM)
OUTSIDE = pl.BlockSpec(memory_space=pltpu.HBM)


def fetch(sources, targets, semaphores):
    copies = [
        pltpu.make_async_copy(source, target, semaphores.at[k])
        for k, (source, target) in enumerate(zip(sources, targets))
    ]
    for copy in copies:
        copy.start()
    return copies


def prepare_body(*refs, capacity):
    sources, outs = refs[:4], refs[4:]
    tail_ref, slots_ref, keys_ref, values_ref, query_ref, routes_ref, semaphores = outs
    targets = (keys_ref, values_ref, routes_ref, query_ref)
    copies = fetch(sources, targets, semaphores)
    for copy in copies:
        copy.wait()
    width, length = keys_ref.shape
    tail_ref[:width, :] = keys_ref[:, length - WINDOW_KEYS :]
    tail_ref[width:, :] = values_ref[:, length - WINDOW_KEYS :]
    experts = lax.axis_size("sp")
    tokens = routes_ref.shape[1]
    numbers = lax.broadcasted_iota(jnp.int32, (experts, tokens), 0)
    named = numbers == routes_ref[0:1, :]
    for choice in range(1, TOP):
        named = named | (numbers == routes_ref[choice : choice + 1, :])
    earlier = lax.broadcasted_iota(jnp.int32, (tokens, tokens), 0) < lax.broadcasted_iota(
        jnp.int32, (tokens, tokens), 1
    )
    ahead = jnp.dot(
        jnp.where(named, 1.0, 0.0).astype(jnp.bfloat16),
        jnp.where(earlier, 1.0, 0.0).astype(jnp.bfloat16),
        preferred_element_type=jnp.float32,
    )
    for choice in range(TOP):
        chosen = routes_ref[choice : choice + 1, :]
        rank = jnp.sum(jnp.where(numbers == chosen, ahead, 0.0), axis=0, keepdims=True)
        relative = chosen ^ lax.axis_index("sp")
        slots_ref[choice : choice + 1, :] = relative * capacity + rank.astype(jnp.int32)


def prepare(keys, values, routes, queries, capacity):
    return pl.pallas_call(
        functools.partial(prepare_body, capacity=capacity),
        in_specs=[OUTSIDE] * 4,
        out_specs=[INSIDE] * 5,
        out_shape=[
            pltpu.VMEM((2 * keys.shape[0], WINDOW_KEYS), keys.dtype),
            pltpu.VMEM(routes.shape, jnp.int32),
            pltpu.VMEM(keys.shape, keys.dtype),
            pltpu.VMEM(values.shape, values.dtype),
            pltpu.VMEM(queries.shape, queries.dtype),
        ],
        scratch_shapes=[
            pltpu.VMEM(routes.shape, routes.dtype),
            pltpu.SemaphoreType.DMA((4,)),
        ],
        compiler_params=pltpu.CompilerParams(vmem_limit_bytes=8 * 2**20),
    )(keys, values, routes, queries)


def attend_block(block, query_ref, before_ref, keys_ref, values_ref, sinks_ref, store):
    width, length = keys_ref.shape
    own = length // lax.axis_size("tp")
    local_heads = query_ref.shape[1] // HEAD_SIZE
    local_kv = width // HEAD_SIZE
    span = own + WINDOW_KEYS
    queries = query_ref[block * own : (block + 1) * own, :]
    if before_ref is None:
        keys, values = keys_ref[:, length - span :], values_ref[:, length - span :]
    else:
        keys, values = [
            jnp.concatenate([before_ref[part * width : (part + 1) * width, :], ref[:, :own]], axis=1)
            for part, ref in enumerate((keys_ref, values_ref))
        ]
    shape = (own, span)
    place = lax.broadcasted_iota(jnp.int32, shape, 1)
    distance = lax.broadcasted_iota(jnp.int32, shape, 0) - place + WINDOW_KEYS
    first = jnp.where(block + lax.axis_index("sp") == 0, WINDOW_KEYS, 0)
    inside = (distance >= 0) & (distance < WINDOW_KEYS) & (place >= first)
    distance = distance.astype(jnp.float32)
    for head in range(local_heads):
        columns = slice(head * HEAD_SIZE, (head + 1) * HEAD_SIZE)
        kv = head * local_kv // local_heads
        rows = slice(kv * HEAD_SIZE, (kv + 1) * HEAD_SIZE)
        slope = jnp.float32(0.0)
        for core in range(lax.axis_size("tp")):
            own_slope = 2.0 ** (-8.0 * (core * local_heads + head + 1.0) / QUERY_HEADS)
            slope = jnp.where(lax.axis_index("tp") == core, jnp.float32(own_slope), slope)
        score = jnp.dot(queries[:, columns], keys[rows, :], preferred_element_type=jnp.float32)
        score = jnp.where(inside, score * HEAD_SIZE ** (-0.5) - slope * distance, -jnp.inf)
        sink = sinks_ref[head]
        peak = jnp.maximum(jnp.max(score, axis=1, keepdims=True), sink)
        weight = jnp.exp(score - peak)
        total = jnp.sum(weight, axis=1, keepdims=True) + jnp.exp(sink - peak)
        probs = (weight / total).astype(jnp.bfloat16)
        store(
            columns,
            lax.dot_general(
                probs,
                values[rows, :],
                (((1,), (1,)), ((), ())),
                preferred_element_type=jnp.float32,
            ).astype(jnp.bfloat16),
        )


def attend_inside_body(*refs):
    query_ref, keys_ref, values_ref, sinks_hbm = refs[:4]
    later, (out_ref, *kept), (sinks_ref, semaphores) = refs[4:8], refs[8:13], refs[13:]
    later = (*later[:-1], later[-1].at[0])
    first, *copies = fetch((sinks_hbm, *later), (sinks_ref, *kept), semaphores)
    first.wait()

    def store(columns, value):
        out_ref[:, columns] = value

    attend_block(1, query_ref, None, keys_ref, values_ref, sinks_ref, store)
    for copy in copies:
        copy.wait()


def attend_border_body(*refs):
    query_ref, before_ref, keys_ref, values_ref, sinks_hbm, inside_ref = refs[:6]
    theirs_ref, mine_ref, sinks_ref, semaphores = refs[6:]
    fetch((sinks_hbm,), (sinks_ref,), semaphores)[0].wait()
    low = lax.axis_index("tp") == 0

    def store(columns, value):
        other = inside_ref[:, columns]
        mine_ref[:, columns] = jnp.where(low, value, other)
        theirs_ref[:, columns] = jnp.where(low, other, value)

    attend_block(0, query_ref, before_ref, keys_ref, values_ref, sinks_ref, store)


def partial_body(rows_ref, weight_ref, residual_ref, sum_ref):
    sum_ref[...] = residual_ref[...].astype(jnp.float32) + jnp.dot(
        rows_ref[...], weight_ref[...], preferred_element_type=jnp.float32
    )


def attend_inside(queries, keys, values, sinks, later, own_rows):
    return pl.pallas_call(
        attend_inside_body,
        in_specs=[INSIDE] * 3 + [OUTSIDE] * 5,
        out_specs=[INSIDE] * 5,
        out_shape=[pltpu.VMEM((own_rows, queries.shape[1]), jnp.bfloat16)]
        + [pltpu.VMEM(x.shape[-2:], x.dtype) for x in later],
        scratch_shapes=[pltpu.SMEM(sinks.shape, sinks.dtype), pltpu.SemaphoreType.DMA((5,))],
        compiler_params=pltpu.CompilerParams(vmem_limit_bytes=16 * 2**20),
    )(queries, keys, values, sinks, *later)


def attend_border(queries, before, keys, values, sinks, inside):
    return pl.pallas_call(
        attend_border_body,
        in_specs=[INSIDE] * 4 + [OUTSIDE, INSIDE],
        out_specs=[INSIDE] * 2,
        out_shape=[jax.ShapeDtypeStruct(inside.shape, inside.dtype)] * 2,
        scratch_shapes=[pltpu.SMEM(sinks.shape, sinks.dtype), pltpu.SemaphoreType.DMA((1,))],
        compiler_params=pltpu.CompilerParams(vmem_limit_bytes=16 * 2**20),
    )(queries, before, keys, values, sinks, inside)


def partial_sum(rows, weight, residual):
    return pl.pallas_call(
        partial_body,
        in_specs=[INSIDE] * 3,
        out_specs=INSIDE,
        out_shape=jax.ShapeDtypeStruct(residual.shape, jnp.float32),
        compiler_params=pltpu.CompilerParams(vmem_limit_bytes=16 * 2**20),
    )(rows, weight, residual)


def project_body(sum_ref, rows_ref, weight_ref, gain_ref, slots_ref, mixed_ref, *out_refs):
    mixed = sum_ref[...] + jnp.dot(
        rows_ref[...], weight_ref[...], preferred_element_type=jnp.float32
    )
    mixed_ref[...] = mixed
    scale = lax.rsqrt(jnp.mean(mixed * mixed, axis=-1, keepdims=True) + 1e-05)
    normed = (mixed * scale * gain_ref[...]).astype(jnp.bfloat16)
    for number, out_ref in enumerate(out_refs):
        shape = (out_ref.shape[0], mixed.shape[0])
        numbers = number * shape[0] + lax.broadcasted_iota(jnp.int32, shape, 0)
        select = numbers == slots_ref[0:1, :]
        for choice in range(1, TOP):
            select = select | (numbers == slots_ref[choice : choice + 1, :])
        out_ref[...] = jnp.dot(
            jnp.where(select, 1.0, 0.0).astype(jnp.bfloat16),
            normed,
            preferred_element_type=jnp.float32,
        ).astype(jnp.bfloat16)


def project(total, rows, weight, gain, slots, group):
    picked = jax.ShapeDtypeStruct((group, total.shape[1]), jnp.bfloat16)
    return pl.pallas_call(
        project_body,
        in_specs=[INSIDE] * 5,
        out_specs=[INSIDE] * (1 + PLANES),
        out_shape=[jax.ShapeDtypeStruct(total.shape, jnp.float32)] + [picked] * PLANES,
        compiler_params=pltpu.CompilerParams(vmem_limit_bytes=16 * 2**20),
    )(total, rows, weight, gain, slots)


BLOCK = 256


def gather_rows(pieces, rows_ref):
    start = 0
    for piece in pieces:
        rows_ref[start : start + piece.shape[0], :] = piece[...]
        start += piece.shape[0]


def load_body(*refs):
    count = len(refs) // 2
    sources = [ref.at[0] for ref in refs[:count]]
    for copy in fetch(sources, refs[count : 2 * count], refs[-1]):
        copy.wait()


def load(*weights):
    return pl.pallas_call(
        load_body,
        in_specs=[OUTSIDE] * len(weights),
        out_specs=[INSIDE] * len(weights),
        out_shape=[pltpu.VMEM(w.shape[1:], w.dtype) for w in weights],
        scratch_shapes=[pltpu.SemaphoreType.DMA((len(weights),))],
        compiler_params=pltpu.CompilerParams(vmem_limit_bytes=4 * 2**20),
    )(*weights)


def expert_body(*refs, count):
    pieces, (gate_ref, up_ref, down_ref, own_ref, other_ref, rows_ref, hidden_ref) = (
        refs[:count],
        refs[count:],
    )
    gather_rows(pieces, rows_ref)
    for start in range(0, gate_ref.shape[1], BLOCK):
        units = slice(start, start + BLOCK)
        rows = rows_ref[...]
        gate = jnp.dot(rows, gate_ref[:, units], preferred_element_type=jnp.float32)
        upper = jnp.dot(rows, up_ref[:, units], preferred_element_type=jnp.float32)
        hidden_ref[:, units] = (gate / (1.0 + jnp.exp(-gate)) * upper).astype(jnp.bfloat16)
    half = own_ref.shape[0]
    for start in range(0, down_ref.shape[1], BLOCK):
        units = slice(start, start + BLOCK)
        part = jnp.dot(
            hidden_ref[...], down_ref[:, units], preferred_element_type=jnp.float32
        ).astype(jnp.bfloat16)
        own_ref[:, units] = part[:half]
        other_ref[:, units] = part[half:]


def expert_parts(pieces, weights):
    width, hidden_units = weights[0].shape
    if any(piece.shape[0] % 8 for piece in pieces):
        pieces = [jnp.concatenate(pieces, axis=0)]
    rows = sum(piece.shape[0] for piece in pieces)
    half = jax.ShapeDtypeStruct((rows // 2, width), jnp.bfloat16)
    inside = pl.BlockSpec(memory_space=pltpu.VMEM)
    return pl.pallas_call(
        functools.partial(expert_body, count=len(pieces)),
        in_specs=[inside] * (len(pieces) + 3),
        out_specs=[inside] * 2,
        out_shape=[half, half],
        scratch_shapes=[
            pltpu.VMEM((rows, width), jnp.bfloat16),
            pltpu.VMEM((rows, hidden_units), jnp.bfloat16),
        ],
        compiler_params=pltpu.CompilerParams(vmem_limit_bytes=8 * 2**20),
        cost_estimate=pl.CostEstimate(
            flops=6 * rows * width * hidden_units,
            transcendentals=rows * hidden_units,
            bytes_accessed=6 * width * hidden_units,
        ),
    )(*pieces, *weights)


def combine_body(*refs, count, base):
    sum_ref, slots_ref, weights_ref = refs[:3]
    pieces, (result_ref, rows_ref) = refs[3 : 3 + count], refs[3 + count :]
    gather_rows(pieces, rows_ref)
    shape = (rows_ref.shape[0], slots_ref.shape[1])
    numbers = base + lax.broadcasted_iota(jnp.int32, shape, 0)
    result = sum_ref[...]
    for choice in range(TOP):
        pick = slots_ref[choice : choice + 1, :] == numbers
        picked = lax.dot_general(
            jnp.where(pick, 1.0, 0.0).astype(jnp.bfloat16),
            rows_ref[...],
            (((0,), (0,)), ((), ())),
            preferred_element_type=jnp.float32,
        )
        result = result + weights_ref[:, choice : choice + 1] * picked
    result_ref[...] = result.astype(result_ref.dtype)


def combine(total, slots, weights, pieces, base, dtype):
    if any(piece.shape[0] % 8 for piece in pieces):
        pieces = [jnp.concatenate(pieces, axis=0)]
    rows = sum(piece.shape[0] for piece in pieces)
    inside = pl.BlockSpec(memory_space=pltpu.VMEM)
    return pl.pallas_call(
        functools.partial(combine_body, count=len(pieces), base=base),
        in_specs=[inside] * (3 + len(pieces)),
        out_specs=inside,
        out_shape=jax.ShapeDtypeStruct(total.shape, dtype),
        scratch_shapes=[pltpu.VMEM((rows, total.shape[1]), jnp.bfloat16)],
        compiler_params=pltpu.CompilerParams(vmem_limit_bytes=8 * 2**20),
        cost_estimate=pl.CostEstimate(
            flops=4 * rows * total.shape[0] * total.shape[1],
            transcendentals=0,
            bytes_accessed=8 * total.shape[0] * total.shape[1],
        ),
    )(total, slots, weights, *pieces)


def on_device(
    query_rows,
    key_rows,
    value_head_rows,
    sink_logit_head,
    out_weight,
    residual,
    norm_gain,
    routes,
    route_weights,
    gate_proj,
    up_proj,
    down_proj,
):
    n_sp = lax.axis_size("sp")
    own_rows = residual.shape[0]
    plane = n_sp // PLANES
    capacity = 3 * own_rows * TOP // (2 * n_sp)
    group = plane * capacity
    outside = [
        pltpu.with_memory_space_constraint(x, pltpu.HBM)
        for x in (
            key_rows.T,
            value_head_rows.T,
            routes.T,
            query_rows,
            sink_logit_head,
        )
    ]
    sinks = outside[4]
    tail, slot_index, keys, values, queries = prepare(*outside[:4], capacity)
    before = from_behind(tail, "sp", 1)
    other_weight = swap_cores(out_weight)
    later = [
        pltpu.with_memory_space_constraint(x, pltpu.HBM)
        for x in (out_weight, residual, norm_gain.reshape(1, -1), gate_proj)
    ]
    inside, own_weight, own_residual, gain, gate_kept = attend_inside(
        queries, keys, values, sinks, later, own_rows
    )
    theirs, mine = attend_border(queries, before, keys, values, sinks, inside)
    from_other = swap_cores(theirs)
    partial = partial_sum(mine, own_weight, own_residual)
    mixed, *selected = project(partial, from_other, other_weight, gain, slot_index, group)
    weights = load(
        *[
            pltpu.with_memory_space_constraint(w, pltpu.HBM)
            for w in (up_proj, down_proj)
        ]
    )
    weights = [pltpu.with_memory_space_constraint(w, pltpu.VMEM) for w in (gate_kept, *weights)]

    def across(block, distance):
        return lax.ppermute(block, "sp", [(i, i ^ distance) for i in range(n_sp)])

    def pieces(block):
        rows = block.shape[0] // plane
        return [block[rows * j : rows * (j + 1)] for j in range(plane)]

    def in_plane(parts):
        return [parts[0]] + [across(parts[j], j) for j in range(1, plane)]

    def expert(parts):
        rows = jnp.concatenate(parts, axis=0)
        other = swap_cores(rows)
        own_part, other_part = expert_parts([rows, other], weights)
        added = swap_cores(other_part)
        return (own_part.astype(jnp.float32) + added.astype(jnp.float32)).astype(jnp.bfloat16)

    arrived = {number: across(selected[number], number * plane) for number in (3, 1, 2)}
    arrived[0] = selected[0]
    out = {number: expert(in_plane(pieces(arrived[number]))) for number in (0, 3, 1, 2)}
    far_back = in_plane(pieces(across(out[3], 3 * plane)))
    zero_back = in_plane(pieces(out[0]))
    one_back = in_plane(pieces(across(out[1], plane)))
    mid_back = [across(p, 2 * plane + j) for j, p in enumerate(pieces(out[2]))]

    total = mixed
    backs = (("zero", 0, zero_back), ("far", 3, far_back), ("one", 1, one_back), ("mid", 2, mid_back))
    for name, number, back in backs:
        dtype = jnp.bfloat16 if name == "mid" else jnp.float32
        total = combine(total, slot_index, route_weights, back, number * group, dtype)
    return total


def solution(mesh):
    placed = (
        P("sp", "tp"),
        P("sp", "tp"),
        P("sp", "tp"),
        P("tp"),
        P("tp", None),
        P(("sp", "tp"), None),
        P(),
        P(("sp", "tp"), None),
        P(("sp", "tp"), None),
        P("sp", None, "tp"),
        P("sp", None, "tp"),
        P("sp", "tp", None),
    )

    return jax.shard_map(
        on_device, mesh=mesh, in_specs=placed, out_specs=P(("sp", "tp"), None), check_vma=False
    )
```

```python
import functools

import jax
import jax.numpy as jnp
from jax import lax
from jax.experimental import pallas as pl
from jax.experimental.pallas import tpu as pltpu
from jax.sharding import PartitionSpec as P


QUERY_HEADS = 16
HEAD_SIZE = 64
TOP = 2
WINDOW_KEYS = 128
PLANES = 4


def from_behind(block, axis, distance):
    devices = range(lax.axis_size(axis))
    route = [(i - distance, i) for i in devices if i - distance in devices]
    return lax.ppermute(block, axis, route)


def swap_cores(block):
    return lax.ppermute(block, "tp", [(0, 1), (1, 0)])


INSIDE = pl.BlockSpec(memory_space=pltpu.VMEM)
OUTSIDE = pl.BlockSpec(memory_space=pltpu.HBM)


def fetch(sources, targets, semaphores):
    copies = [
        pltpu.make_async_copy(source, target, semaphores.at[k])
        for k, (source, target) in enumerate(zip(sources, targets))
    ]
    for copy in copies:
        copy.start()
    return copies


def prepare_body(*refs, capacity):
    sources, outs = refs[:4], refs[4:]
    tail_ref, slots_ref, keys_ref, values_ref, query_ref, routes_ref, semaphores = outs
    targets = (keys_ref, values_ref, routes_ref, query_ref)
    copies = fetch(sources, targets, semaphores)
    for copy in copies:
        copy.wait()
    width, length = keys_ref.shape
    tail_ref[:width, :] = keys_ref[:, length - WINDOW_KEYS :]
    tail_ref[width:, :] = values_ref[:, length - WINDOW_KEYS :]
    experts = lax.axis_size("sp")
    tokens = routes_ref.shape[1]
    numbers = lax.broadcasted_iota(jnp.int32, (experts, tokens), 0)
    named = numbers == routes_ref[0:1, :]
    for choice in range(1, TOP):
        named = named | (numbers == routes_ref[choice : choice + 1, :])
    earlier = lax.broadcasted_iota(jnp.int32, (tokens, tokens), 0) < lax.broadcasted_iota(
        jnp.int32, (tokens, tokens), 1
    )
    ahead = jnp.dot(
        jnp.where(named, 1.0, 0.0).astype(jnp.bfloat16),
        jnp.where(earlier, 1.0, 0.0).astype(jnp.bfloat16),
        preferred_element_type=jnp.float32,
    )
    for choice in range(TOP):
        chosen = routes_ref[choice : choice + 1, :]
        rank = jnp.sum(jnp.where(numbers == chosen, ahead, 0.0), axis=0, keepdims=True)
        relative = chosen ^ lax.axis_index("sp")
        slots_ref[choice : choice + 1, :] = relative * capacity + rank.astype(jnp.int32)


def prepare(keys, values, routes, queries, capacity):
    return pl.pallas_call(
        functools.partial(prepare_body, capacity=capacity),
        in_specs=[OUTSIDE] * 4,
        out_specs=[INSIDE] * 5,
        out_shape=[
            pltpu.VMEM((2 * keys.shape[0], WINDOW_KEYS), keys.dtype),
            pltpu.VMEM(routes.shape, jnp.int32),
            pltpu.VMEM(keys.shape, keys.dtype),
            pltpu.VMEM(values.shape, values.dtype),
            pltpu.VMEM(queries.shape, queries.dtype),
        ],
        scratch_shapes=[
            pltpu.VMEM(routes.shape, routes.dtype),
            pltpu.SemaphoreType.DMA((4,)),
        ],
        compiler_params=pltpu.CompilerParams(vmem_limit_bytes=8 * 2**20),
    )(keys, values, routes, queries)


def attend_block(block, query_ref, before_ref, keys_ref, values_ref, sinks_ref, store):
    width, length = keys_ref.shape
    own = length // lax.axis_size("tp")
    local_heads = query_ref.shape[1] // HEAD_SIZE
    local_kv = width // HEAD_SIZE
    span = own + WINDOW_KEYS
    queries = query_ref[block * own : (block + 1) * own, :]
    if before_ref is None:
        keys, values = keys_ref[:, length - span :], values_ref[:, length - span :]
    else:
        keys, values = [
            jnp.concatenate([before_ref[part * width : (part + 1) * width, :], ref[:, :own]], axis=1)
            for part, ref in enumerate((keys_ref, values_ref))
        ]
    shape = (own, span)
    place = lax.broadcasted_iota(jnp.int32, shape, 1)
    distance = lax.broadcasted_iota(jnp.int32, shape, 0) - place + WINDOW_KEYS
    first = jnp.where(block + lax.axis_index("sp") == 0, WINDOW_KEYS, 0)
    inside = (distance >= 0) & (distance < WINDOW_KEYS) & (place >= first)
    distance = distance.astype(jnp.float32)
    for head in range(local_heads):
        columns = slice(head * HEAD_SIZE, (head + 1) * HEAD_SIZE)
        kv = head * local_kv // local_heads
        rows = slice(kv * HEAD_SIZE, (kv + 1) * HEAD_SIZE)
        slope = jnp.float32(0.0)
        for core in range(lax.axis_size("tp")):
            own_slope = 2.0 ** (-8.0 * (core * local_heads + head + 1.0) / QUERY_HEADS)
            slope = jnp.where(lax.axis_index("tp") == core, jnp.float32(own_slope), slope)
        score = jnp.dot(queries[:, columns], keys[rows, :], preferred_element_type=jnp.float32)
        score = jnp.where(inside, score * HEAD_SIZE ** (-0.5) - slope * distance, -jnp.inf)
        sink = sinks_ref[head]
        peak = jnp.maximum(jnp.max(score, axis=1, keepdims=True), sink)
        weight = jnp.exp(score - peak)
        total = jnp.sum(weight, axis=1, keepdims=True) + jnp.exp(sink - peak)
        probs = (weight / total).astype(jnp.bfloat16)
        store(
            columns,
            lax.dot_general(
                probs,
                values[rows, :],
                (((1,), (1,)), ((), ())),
                preferred_element_type=jnp.float32,
            ).astype(jnp.bfloat16),
        )


def attend_inside_body(*refs):
    query_ref, keys_ref, values_ref, sinks_hbm = refs[:4]
    later, (out_ref, *kept), (sinks_ref, semaphores) = refs[4:8], refs[8:13], refs[13:]
    later = (*later[:-1], later[-1].at[0])
    first, *copies = fetch((sinks_hbm, *later), (sinks_ref, *kept), semaphores)
    first.wait()

    def store(columns, value):
        out_ref[:, columns] = value

    attend_block(1, query_ref, None, keys_ref, values_ref, sinks_ref, store)
    for copy in copies:
        copy.wait()


def attend_border_body(*refs):
    query_ref, before_ref, keys_ref, values_ref, sinks_hbm, inside_ref = refs[:6]
    theirs_ref, mine_ref, sinks_ref, semaphores = refs[6:]
    fetch((sinks_hbm,), (sinks_ref,), semaphores)[0].wait()
    low = lax.axis_index("tp") == 0

    def store(columns, value):
        other = inside_ref[:, columns]
        mine_ref[:, columns] = jnp.where(low, value, other)
        theirs_ref[:, columns] = jnp.where(low, other, value)

    attend_block(0, query_ref, before_ref, keys_ref, values_ref, sinks_ref, store)


def partial_body(rows_ref, weight_ref, residual_ref, sum_ref):
    sum_ref[...] = residual_ref[...].astype(jnp.float32) + jnp.dot(
        rows_ref[...], weight_ref[...], preferred_element_type=jnp.float32
    )


def attend_inside(queries, keys, values, sinks, later, own_rows):
    return pl.pallas_call(
        attend_inside_body,
        in_specs=[INSIDE] * 3 + [OUTSIDE] * 5,
        out_specs=[INSIDE] * 5,
        out_shape=[pltpu.VMEM((own_rows, queries.shape[1]), jnp.bfloat16)]
        + [pltpu.VMEM(x.shape[-2:], x.dtype) for x in later],
        scratch_shapes=[pltpu.SMEM(sinks.shape, sinks.dtype), pltpu.SemaphoreType.DMA((5,))],
        compiler_params=pltpu.CompilerParams(vmem_limit_bytes=16 * 2**20),
    )(queries, keys, values, sinks, *later)


def attend_border(queries, before, keys, values, sinks, inside):
    return pl.pallas_call(
        attend_border_body,
        in_specs=[INSIDE] * 4 + [OUTSIDE, INSIDE],
        out_specs=[INSIDE] * 2,
        out_shape=[jax.ShapeDtypeStruct(inside.shape, inside.dtype)] * 2,
        scratch_shapes=[pltpu.SMEM(sinks.shape, sinks.dtype), pltpu.SemaphoreType.DMA((1,))],
        compiler_params=pltpu.CompilerParams(vmem_limit_bytes=16 * 2**20),
    )(queries, before, keys, values, sinks, inside)


def partial_sum(rows, weight, residual):
    return pl.pallas_call(
        partial_body,
        in_specs=[INSIDE] * 3,
        out_specs=INSIDE,
        out_shape=jax.ShapeDtypeStruct(residual.shape, jnp.float32),
        compiler_params=pltpu.CompilerParams(vmem_limit_bytes=16 * 2**20),
    )(rows, weight, residual)


def project_body(sum_ref, rows_ref, weight_ref, gain_ref, slots_ref, mixed_ref, *out_refs):
    mixed = sum_ref[...] + jnp.dot(
        rows_ref[...], weight_ref[...], preferred_element_type=jnp.float32
    )
    mixed_ref[...] = mixed
    scale = lax.rsqrt(jnp.mean(mixed * mixed, axis=-1, keepdims=True) + 1e-05)
    normed = (mixed * scale * gain_ref[...]).astype(jnp.bfloat16)
    for number, out_ref in enumerate(out_refs):
        shape = (out_ref.shape[0], mixed.shape[0])
        numbers = number * shape[0] + lax.broadcasted_iota(jnp.int32, shape, 0)
        select = numbers == slots_ref[0:1, :]
        for choice in range(1, TOP):
            select = select | (numbers == slots_ref[choice : choice + 1, :])
        out_ref[...] = jnp.dot(
            jnp.where(select, 1.0, 0.0).astype(jnp.bfloat16),
            normed,
            preferred_element_type=jnp.float32,
        ).astype(jnp.bfloat16)


def project(total, rows, weight, gain, slots, group):
    picked = jax.ShapeDtypeStruct((group, total.shape[1]), jnp.bfloat16)
    return pl.pallas_call(
        project_body,
        in_specs=[INSIDE] * 5,
        out_specs=[INSIDE] * (1 + PLANES),
        out_shape=[jax.ShapeDtypeStruct(total.shape, jnp.float32)] + [picked] * PLANES,
        compiler_params=pltpu.CompilerParams(vmem_limit_bytes=16 * 2**20),
    )(total, rows, weight, gain, slots)


BLOCK = 256


def gather_rows(pieces, rows_ref):
    start = 0
    for piece in pieces:
        rows_ref[start : start + piece.shape[0], :] = piece[...]
        start += piece.shape[0]


def load_body(*refs):
    count = len(refs) // 2
    sources = [ref.at[0] for ref in refs[:count]]
    for copy in fetch(sources, refs[count : 2 * count], refs[-1]):
        copy.wait()


def load(*weights):
    return pl.pallas_call(
        load_body,
        in_specs=[OUTSIDE] * len(weights),
        out_specs=[INSIDE] * len(weights),
        out_shape=[pltpu.VMEM(w.shape[1:], w.dtype) for w in weights],
        scratch_shapes=[pltpu.SemaphoreType.DMA((len(weights),))],
        compiler_params=pltpu.CompilerParams(vmem_limit_bytes=4 * 2**20),
    )(*weights)


def expert_body(*refs, count):
    pieces, (gate_ref, up_ref, down_ref, own_ref, other_ref, rows_ref, hidden_ref) = (
        refs[:count],
        refs[count:],
    )
    gather_rows(pieces, rows_ref)
    for start in range(0, gate_ref.shape[1], BLOCK):
        units = slice(start, start + BLOCK)
        rows = rows_ref[...]
        gate = jnp.dot(rows, gate_ref[:, units], preferred_element_type=jnp.float32)
        upper = jnp.dot(rows, up_ref[:, units], preferred_element_type=jnp.float32)
        hidden_ref[:, units] = (gate / (1.0 + jnp.exp(-gate)) * upper).astype(jnp.bfloat16)
    half = own_ref.shape[0]
    for start in range(0, down_ref.shape[1], BLOCK):
        units = slice(start, start + BLOCK)
        part = jnp.dot(
            hidden_ref[...], down_ref[:, units], preferred_element_type=jnp.float32
        ).astype(jnp.bfloat16)
        own_ref[:, units] = part[:half]
        other_ref[:, units] = part[half:]


def expert_parts(pieces, weights):
    width, hidden_units = weights[0].shape
    if any(piece.shape[0] % 8 for piece in pieces):
        pieces = [jnp.concatenate(pieces, axis=0)]
    rows = sum(piece.shape[0] for piece in pieces)
    half = jax.ShapeDtypeStruct((rows // 2, width), jnp.bfloat16)
    inside = pl.BlockSpec(memory_space=pltpu.VMEM)
    return pl.pallas_call(
        functools.partial(expert_body, count=len(pieces)),
        in_specs=[inside] * (len(pieces) + 3),
        out_specs=[inside] * 2,
        out_shape=[half, half],
        scratch_shapes=[
            pltpu.VMEM((rows, width), jnp.bfloat16),
            pltpu.VMEM((rows, hidden_units), jnp.bfloat16),
        ],
        compiler_params=pltpu.CompilerParams(vmem_limit_bytes=8 * 2**20),
        cost_estimate=pl.CostEstimate(
            flops=6 * rows * width * hidden_units,
            transcendentals=rows * hidden_units,
            bytes_accessed=6 * width * hidden_units,
        ),
    )(*pieces, *weights)


def combine_body(*refs, count, base):
    sum_ref, slots_ref, weights_ref = refs[:3]
    pieces, (result_ref, rows_ref) = refs[3 : 3 + count], refs[3 + count :]
    gather_rows(pieces, rows_ref)
    shape = (rows_ref.shape[0], slots_ref.shape[1])
    numbers = base + lax.broadcasted_iota(jnp.int32, shape, 0)
    result = sum_ref[...]
    tokens = slots_ref.shape[1]
    diagonal = lax.broadcasted_iota(jnp.int32, (tokens, tokens), 0) == lax.broadcasted_iota(
        jnp.int32, (tokens, tokens), 1
    )
    for choice in range(TOP):
        spread = jnp.where(diagonal, weights_ref[choice : choice + 1, :], 0.0)
        weight = jnp.sum(spread, axis=1, keepdims=True)
        pick = slots_ref[choice : choice + 1, :] == numbers
        picked = lax.dot_general(
            jnp.where(pick, 1.0, 0.0).astype(jnp.bfloat16),
            rows_ref[...],
            (((0,), (0,)), ((), ())),
            preferred_element_type=jnp.float32,
        )
        result = result + weight * picked
    result_ref[...] = result.astype(result_ref.dtype)


def combine(total, slots, weights, pieces, base, dtype):
    if any(piece.shape[0] % 8 for piece in pieces):
        pieces = [jnp.concatenate(pieces, axis=0)]
    rows = sum(piece.shape[0] for piece in pieces)
    inside = pl.BlockSpec(memory_space=pltpu.VMEM)
    return pl.pallas_call(
        functools.partial(combine_body, count=len(pieces), base=base),
        in_specs=[inside] * (3 + len(pieces)),
        out_specs=inside,
        out_shape=jax.ShapeDtypeStruct(total.shape, dtype),
        scratch_shapes=[pltpu.VMEM((rows, total.shape[1]), jnp.bfloat16)],
        compiler_params=pltpu.CompilerParams(vmem_limit_bytes=8 * 2**20),
        cost_estimate=pl.CostEstimate(
            flops=4 * rows * total.shape[0] * total.shape[1],
            transcendentals=0,
            bytes_accessed=8 * total.shape[0] * total.shape[1],
        ),
    )(total, slots, weights, *pieces)


def on_device(
    query_rows,
    key_rows,
    value_head_rows,
    sink_logit_head,
    out_weight,
    residual,
    norm_gain,
    routes,
    route_weights,
    gate_proj,
    up_proj,
    down_proj,
):
    n_sp = lax.axis_size("sp")
    own_rows = residual.shape[0]
    plane = n_sp // PLANES
    capacity = 3 * own_rows * TOP // (2 * n_sp)
    group = plane * capacity
    outside = [
        pltpu.with_memory_space_constraint(x, pltpu.HBM)
        for x in (
            key_rows.T,
            value_head_rows.T,
            routes.T,
            query_rows,
            sink_logit_head,
        )
    ]
    sinks = outside[4]
    tail, slot_index, keys, values, queries = prepare(*outside[:4], capacity)
    before = from_behind(tail, "sp", 1)
    other_weight = swap_cores(out_weight)
    later = [
        pltpu.with_memory_space_constraint(x, pltpu.HBM)
        for x in (out_weight, residual, norm_gain.reshape(1, -1), gate_proj)
    ]
    inside, own_weight, own_residual, gain, gate_kept = attend_inside(
        queries, keys, values, sinks, later, own_rows
    )
    theirs, mine = attend_border(queries, before, keys, values, sinks, inside)
    from_other = swap_cores(theirs)
    partial = partial_sum(mine, own_weight, own_residual)
    mixed, *selected = project(partial, from_other, other_weight, gain, slot_index, group)
    weights = load(
        *[
            pltpu.with_memory_space_constraint(w, pltpu.HBM)
            for w in (up_proj, down_proj)
        ]
    )
    weights = [pltpu.with_memory_space_constraint(w, pltpu.VMEM) for w in (gate_kept, *weights)]

    def across(block, distance):
        return lax.ppermute(block, "sp", [(i, i ^ distance) for i in range(n_sp)])

    def pieces(block):
        rows = block.shape[0] // plane
        return [block[rows * j : rows * (j + 1)] for j in range(plane)]

    def in_plane(parts):
        return [parts[0]] + [across(parts[j], j) for j in range(1, plane)]

    def expert(parts):
        rows = jnp.concatenate(parts, axis=0)
        other = swap_cores(rows)
        own_part, other_part = expert_parts([rows, other], weights)
        added = swap_cores(other_part)
        return (own_part.astype(jnp.float32) + added.astype(jnp.float32)).astype(jnp.bfloat16)

    arrived = {number: across(selected[number], number * plane) for number in (3, 1, 2)}
    arrived[0] = selected[0]
    out = {number: expert(in_plane(pieces(arrived[number]))) for number in (0, 3, 1, 2)}
    far_back = in_plane(pieces(across(out[3], 3 * plane)))
    zero_back = in_plane(pieces(out[0]))
    one_back = in_plane(pieces(across(out[1], plane)))
    mid_back = [across(p, 2 * plane + j) for j, p in enumerate(pieces(out[2]))]

    total = mixed
    backs = (("zero", 0, zero_back), ("far", 3, far_back), ("one", 1, one_back), ("mid", 2, mid_back))
    for name, number, back in backs:
        dtype = jnp.bfloat16 if name == "mid" else jnp.float32
        total = combine(total, slot_index, route_weights.T, back, number * group, dtype)
    return total


def solution(mesh):
    placed = (
        P("sp", "tp"),
        P("sp", "tp"),
        P("sp", "tp"),
        P("tp"),
        P("tp", None),
        P(("sp", "tp"), None),
        P(),
        P(("sp", "tp"), None),
        P(("sp", "tp"), None),
        P("sp", None, "tp"),
        P("sp", None, "tp"),
        P("sp", "tp", None),
    )

    return jax.shard_map(
        on_device, mesh=mesh, in_specs=placed, out_specs=P(("sp", "tp"), None), check_vma=False
    )
```
